32 devices in a mesh: ep: 16 (over z, y, x), tp: 2 (over core).
Axes of the slice: x: 2, y: 2, z: 4, core: 2. Of those that a mesh axis runs over, the one named last changes fastest.
Arguments:
- tokens: bfloat16 [384, 4096], P('ep'), may hold values from -6 to 6
- in_gain: float32 [4096], replicated, may hold values from 0.1 to 1.9
- routes: int32 [384, 6], P('ep'), may hold values from 0 to 15, all different within a row; in each aligned block of 24 rows (0 to 23, 24 to 47, ...) at most 10 rows name the same one
- gates: float32 [384, 6], P('ep'), may hold values from 0.25 to 1.5
- expert_gate: bfloat16 [16, 512, 4096], P('ep', 'tp'), may hold values from -0.09375 to 0.09375
- expert_up: bfloat16 [16, 512, 4096], P('ep', 'tp'), may hold values from -0.09375 to 0.09375
- expert_down: bfloat16 [16, 512, 4096], P('ep', None, 'tp'), may hold values from -0.25 to 0.25
- shared_gate: bfloat16 [512, 4096], P('tp'), may hold values from -0.09375 to 0.09375
- shared_up: bfloat16 [512, 4096], P('tp'), may hold values from -0.09375 to 0.09375
- shared_down: bfloat16 [512, 4096], P(None, 'tp')
- out_gain: float32 [4096], P('tp'), may hold values from 0.1 to 1.9
Outputs:
- mixed: bfloat16 [384, 4096], P('ep', 'tp')
The draws below stay inside these ranges and needn't reach their ends.
Inputs may be any that keep to these rules, and one draw needn't show every extreme that they name: `routes`: each row names 6 different experts; among the 24 rows of one index of ep no expert is named more than 10 times, and on some index of ep some expert is named exactly 10 times.
All inputs are finite; a program needn't handle non-finite values.
Results may differ from the reference program's by a relative error of at most 0.0075.
Values may be sent and summed in bfloat16 or wider, within the bound.
A program may use at most 64 MiB of HBM per device.

```python
import math
import jax
import jax.numpy as jnp
import numpy as np
from jax import lax

D = 4096
FF = 512
SF = 512
TOPK = 6
TOK_DEV = 24
EXPERTS = 16
TOKENS = 384
CAP = 10


def draw_shared_down(key, part):
    block_width = min(128, D)
    blocks = D // block_width
    first, second = jax.random.split(jax.random.fold_in(key, 11))
    scales = jnp.exp(jax.random.uniform(first, (blocks,), jnp.float32, -1.2, 1.2))
    column_scale = jnp.repeat(scales, block_width)
    values = jax.random.normal(second, (SF, D), jnp.float32) * SF ** (-0.5)
    return (values * column_scale[None, :]).astype(jnp.bfloat16)


def steps_of(stream_key, shape, pieces, smallest, high):
    def one(axis_at, blocks):
        draws = jax.random.uniform(jax.random.fold_in(jax.random.fold_in(stream_key, 6), axis_at), (blocks,), jnp.float32, smallest / len(pieces), high / len(pieces))
        return jnp.repeat(jnp.exp(draws), shape[axis_at] // blocks).reshape((-1,) + (1,) * (len(shape) - axis_at - 1))

    factor_of = one(*pieces[0])
    for cut in pieces[1:]:
        factor_of = factor_of * one(*cut)
    return factor_of


def deal_out(rng, own, number, rows, number_of, top, limit, skew):
    ranking = jax.random.permutation(rng, number_of)
    packed, common = load_shares(number_of, rows * top, limit, skew, True), load_shares(number_of, rows * top, limit, skew, False)
    places = jnp.arange(number_of)

    def named(tallies, offset_by):
        used = int((tallies > 0).sum())
        fixed = max(1, used // 4)
        shifted = fixed + (places - fixed + offset_by * (used - fixed)) % max(1, number_of - fixed)
        return jnp.zeros((number_of,), jnp.int32).at[ranking[jnp.where(places < fixed, places, shifted)]].set(jnp.asarray(tallies, jnp.int32))

    tallies = jnp.where(number % 4 == 0, named(packed, number // 4), named(common, number - number // 4 - 1))
    mixed = jax.random.permutation(jax.random.fold_in(own, 3), number_of)
    source_of, taker = mixed[0:number_of // 2 * 2:2], mixed[1:number_of // 2 * 2:2]
    slack = jnp.minimum(tallies[source_of] - 1, limit - tallies[taker]) // 2
    slack = jnp.where((source_of == ranking[0]) | (taker == ranking[0]) | (tallies[taker] == 0), 0, jnp.maximum(slack, 0))
    shifted = jax.random.randint(jax.random.fold_in(own, 4), (number_of // 2,), 0, 1 << 20) % (slack + 1)
    tallies = tallies.at[source_of].add(-shifted).at[taker].add(shifted)
    members = jnp.searchsorted(jnp.cumsum(tallies), jnp.arange(rows * top), side="right").astype(jnp.int32)
    listing = members.reshape(top, rows).T
    listing = listing[jax.random.permutation(jax.random.fold_in(own, 1), rows)]
    offset_by = jax.random.randint(jax.random.fold_in(own, 2), (rows, 1), 0, top)
    return jnp.take_along_axis(listing, (jnp.arange(top)[None, :] + offset_by) % top, axis=1)


def load_shares(number_of, total, reach, lean, full):
    weights = [(1 << 20) // math.isqrt(grade ** lean) + 1 for grade in range(1, number_of + 1)]
    largest = reach if full else min(reach, max(-(-total // number_of), total * weights[0] // sum(weights)))
    least = 1 if total - largest >= number_of - 1 else 0
    given, surplus = [largest] + [least] * (number_of - 1), total - largest - least * (number_of - 1)
    while surplus > 0:
        free = [i for i in range(1, number_of) if given[i] < largest] or [i for i in range(1, number_of) if given[i] < reach]
        mass, remaining = sum([weights[i] for i in free]), surplus
        for i in free:
            extra = min(reach - given[i], max(1, remaining * weights[i] // mass), surplus)
            given[i] = given[i] + extra
            surplus = surplus - extra
    return np.array(given)


def scatter_about(own_key, dims, spread, reach, shards=(), held_as=jnp.bfloat16):
    factor_of = steps_of(own_key, dims, shards, -0.22, 0.18) if shards else 1.0
    array = jax.random.normal(own_key, dims, jnp.float32) * spread * factor_of
    return jnp.minimum(jnp.maximum(array, -reach), reach).astype(held_as)


def setup_inputs(seed: int = 0) -> dict:
    streams_of = jax.random.split(jax.random.key(seed), 12)
    tokens = scatter_about(streams_of[0], (TOKENS, D), 1.0, 6.0, ((0, 16),))
    in_gain = jnp.clip(1.0 + 0.18 * jax.random.normal(streams_of[1], (D,), jnp.float32), 0.1, 1.9)
    routes_keys = jax.random.split(jax.random.fold_in(streams_of[2], 1), TOKENS // TOK_DEV)
    routes_turns = jax.random.permutation(jax.random.fold_in(streams_of[2], 3), TOKENS // TOK_DEV)
    routes = jax.vmap(lambda own, number: deal_out(jax.random.fold_in(streams_of[2], 2), own, number, TOK_DEV, EXPERTS, TOPK, CAP, 2))(routes_keys, routes_turns).reshape((TOKENS, TOPK))
    gates = jnp.clip(0.25 + 1.25 * jax.random.uniform(streams_of[3], (TOKENS, TOPK), jnp.float32) ** steps_of(streams_of[3], (TOKENS, TOPK), ((0, 16),), -0.2, 0.2), 0.25, 1.5)
    expert_gate = scatter_about(streams_of[4], (EXPERTS, FF, D), D ** -0.5, 0.09375, ((0, 16), (1, 2)))
    expert_up = scatter_about(streams_of[5], (EXPERTS, FF, D), D ** -0.5, 0.09375, ((0, 16), (1, 2)))
    expert_down = scatter_about(streams_of[6], (EXPERTS, FF, D), FF ** -0.5, 0.25, ((0, 16), (2, 2)))
    shared_gate = scatter_about(streams_of[7], (SF, D), D ** -0.5, 0.09375, ((0, 2),))
    shared_up = scatter_about(streams_of[8], (SF, D), D ** -0.5, 0.09375, ((0, 2),))
    shared_down = draw_shared_down(jax.random.fold_in(streams_of[11], 71), 0)
    out_gain = jnp.clip(1.0 + 0.18 * jax.random.normal(streams_of[10], (D,), jnp.float32), 0.1, 1.9)
    return dict(tokens=tokens, in_gain=in_gain, routes=routes, gates=gates, expert_gate=expert_gate, expert_up=expert_up, expert_down=expert_down, shared_gate=shared_gate, shared_up=shared_up, shared_down=shared_down, out_gain=out_gain)


EPS = 1e-06

def norm_rows(values, gain):
    return values * lax.rsqrt(lax.optimization_barrier(jnp.mean(values * values, axis=1, keepdims=True)) + EPS) * gain

def project(rows, weight):
    return lax.dot_general(rows, weight, (((1,), (1,)), ((), ())), preferred_element_type=jnp.float32)

def reference(tokens, in_gain, routes, gates, expert_gate, expert_up, expert_down, shared_gate, shared_up, shared_down, out_gain):
    normed = norm_rows(tokens.astype(jnp.float32), in_gain.astype(jnp.float32)).astype(jnp.bfloat16)
    shared_hidden = (jax.nn.silu(project(normed, shared_gate)) * project(normed, shared_up)).astype(jnp.bfloat16)
    shared_out = jnp.dot(shared_hidden, shared_down, preferred_element_type=jnp.float32)

    def expert_step(running, inputs):
        w_gate, w_up, w_down, index = inputs
        hidden = (jax.nn.silu(project(normed, w_gate)) * project(normed, w_up)).astype(jnp.bfloat16)
        outputs = jnp.dot(hidden, w_down, preferred_element_type=jnp.float32).astype(jnp.bfloat16)
        weight = lax.optimization_barrier(jnp.sum(jnp.where(routes == index, gates, 0.0), axis=1))
        return (running + weight[:, None] * outputs.astype(jnp.float32), None)
    start = jnp.zeros((tokens.shape[0], tokens.shape[1]), jnp.float32)
    routed, _ = lax.scan(expert_step, start, (expert_gate, expert_up, expert_down, jnp.arange(EXPERTS, dtype=jnp.int32)))
    combined = routed + shared_out
    return norm_rows(combined, out_gain.astype(jnp.float32)).astype(jnp.bfloat16)
```

```python
import functools

import jax
import jax.numpy as jnp
from jax import lax
from jax.experimental import pallas as pl
from jax.experimental.pallas import tpu as pltpu
from jax.sharding import PartitionSpec as P

EPS = 1e-06
MESH = pl.DeviceIdType.MESH
F32 = jnp.float32
BF16 = jnp.bfloat16


def dot_nt(a, b):
    return lax.dot_general(a, b, (((1,), (1,)), ((), ())), preferred_element_type=F32)


def dot_nn(a, b):
    return jnp.dot(a, b, preferred_element_type=F32)


def silu_mul(g, u):
    return g / (1.0 + jnp.exp(-g)) * u


def kernel(
    experts, cap, pad,
    tok, ing, routes, gates, eg, eu, ed, sg, su, sd, outg,
    o,
    vg, vu, vd, vsg, vsu, vsd,
    nrm, send, recv, acc_g, acc_u, sacc_g, sacc_u, hbuf, shbuf, outb, ret, comb, sq,
    wsem, lsem, dsend, drecv, fsend, frecv, rsend, rrecv, xsend, xrecv,
):
    me = lax.axis_index("ep")
    tp = lax.axis_index("tp")
    rows, width = tok.shape
    group = lax.axis_size("tp")
    half = width // group
    slots = experts * pad
    kc = min(512, half)

    loads = [
        pltpu.make_async_copy(src, dst, wsem.at[i])
        for i, (src, dst) in enumerate(
            ((sg, vsg), (su, vsu), (eg.at[0], vg), (eu.at[0], vu), (ed.at[0], vd), (sd, vsd))
        )
    ]
    for load in loads:
        load.start()

    ret[...] = jnp.zeros_like(ret)

    barrier = pltpu.get_barrier_semaphore()

    @pl.loop(1, experts)
    def _(k):
        pl.semaphore_signal(
            barrier, inc=1, device_id=(lax.rem(me + k, experts), tp), device_id_type=MESH
        )

    for q in range(1, group):
        pl.semaphore_signal(
            barrier, inc=1, device_id=(me, lax.rem(tp + q, group)), device_id_type=MESH
        )

    x = tok[...].astype(F32)
    scale = lax.rsqrt(jnp.mean(x * x, axis=1, keepdims=True) + EPS)
    for h in range(group):
        cols = slice(h * half, (h + 1) * half)
        nrm[h] = (tok[:, cols].astype(F32) * scale * ing[:, cols]).astype(BF16)

    expert_ids = lax.broadcasted_iota(jnp.int32, (rows, experts), 1)
    chosen = jnp.zeros((rows, experts), F32)
    weight = jnp.zeros((rows, experts), F32)
    for k in range(routes.shape[1]):
        hit = routes[:, k : k + 1] == expert_ids
        chosen = jnp.where(hit, 1.0, chosen)
        weight = jnp.where(hit, gates[:, k : k + 1], weight)
    chosen = chosen.astype(BF16)
    earlier = (
        lax.broadcasted_iota(jnp.int32, (rows, rows), 1)
        < lax.broadcasted_iota(jnp.int32, (rows, rows), 0)
    ).astype(F32).astype(BF16)
    rank = dot_nn(earlier, chosen).astype(BF16)
    slot_r = lax.broadcasted_iota(jnp.int32, (slots, experts), 0)
    spread_t = (
        slot_r // pad == lax.broadcasted_iota(jnp.int32, (slots, experts), 1)
    ).astype(F32).astype(BF16)
    place_r = (lax.broadcasted_iota(jnp.int32, (slots, rows), 0) % pad).astype(F32)
    placing = jnp.where(
        (dot_nt(spread_t, chosen) > 0.5) & (dot_nt(spread_t, rank) == place_r), 1.0, 0.0
    ).astype(BF16)
    for c in range(half // kc):
        cols = slice(c * kc, (c + 1) * kc)
        send[:, :, cols] = (
            dot_nn(placing, nrm[tp, :, cols]).astype(BF16).reshape(experts, pad, kc)
        )

    pl.semaphore_wait(barrier, experts - 1 + group - 1)

    def dispatch(dest, source):
        return pltpu.make_async_remote_copy(
            src_ref=send.at[dest],
            dst_ref=recv.at[tp, source],
            send_sem=dsend.at[dest],
            recv_sem=drecv.at[source],
            device_id=(dest, tp),
            device_id_type=MESH,
        )

    def forward(part, source, q):
        return pltpu.make_async_remote_copy(
            src_ref=recv.at[part, source],
            dst_ref=recv.at[part, source],
            send_sem=fsend.at[q, source],
            recv_sem=frecv.at[part, source],
            device_id=(me, lax.rem(tp + q, group)),
            device_id_type=MESH,
        )

    def give_back(dest, source):
        return pltpu.make_async_remote_copy(
            src_ref=outb.at[dest],
            dst_ref=ret.at[source],
            send_sem=rsend.at[dest],
            recv_sem=rrecv.at[source],
            device_id=(dest, tp),
            device_id_type=MESH,
        )

    def swap(ref, i, part, q):
        return pltpu.make_async_remote_copy(
            src_ref=ref.at[part],
            dst_ref=ref.at[part],
            send_sem=xsend.at[i, q],
            recv_sem=xrecv.at[i, part],
            device_id=(me, lax.rem(tp + q, group)),
            device_id_type=MESH,
        )

    def swap_start(ref, i):
        for q in range(1, group):
            swap(ref, i, tp, q).start()

    def swap_recv(ref, i):
        for q in range(1, group):
            swap(ref, i, lax.rem(tp + q, group), q).wait_recv()

    def swap_sent(ref, i):
        for q in range(1, group):
            swap(ref, i, tp, q).wait_send()

    def forward_start(source):
        for q in range(1, group):
            forward(tp, source, q).start()

    @pl.loop(1, experts)
    def _(k):
        dispatch(lax.rem(me + k, experts), me).start()

    own = pltpu.make_async_copy(
        send.at[me], recv.at[tp, me], lsem.at[0]
    )
    own.start()

    loads[0].wait()
    loads[1].wait()
    sacc_g[...] = jnp.zeros_like(sacc_g)
    sacc_u[...] = jnp.zeros_like(sacc_u)
    for h in range(group):

        @pl.loop(0, half // kc)
        def _(c):
            cols = pl.ds(pl.multiple_of(c * kc, kc), kc)
            wide = pl.ds(pl.multiple_of(h * half + c * kc, kc), kc)
            xs = nrm[h, :, cols]
            sacc_g[...] += dot_nt(xs, vsg[:, wide])
            sacc_u[...] += dot_nt(xs, vsu[:, wide])

    shbuf[tp] = silu_mul(sacc_g[...], sacc_u[...]).astype(BF16)
    swap_start(shbuf, 0)

    own.wait()
    forward_start(me)

    @pl.loop(1, experts)
    def _(k):
        source = lax.rem(me + experts - k, experts)
        dispatch(source, source).wait_recv()
        forward_start(source)

    loads[2].wait()
    loads[3].wait()
    acc_g[...] = jnp.zeros_like(acc_g)
    acc_u[...] = jnp.zeros_like(acc_u)

    def project_part(part):
        @pl.loop(0, half // kc)
        def _(c):
            cols = pl.ds(pl.multiple_of(c * kc, kc), kc)
            wide = pl.ds(pl.multiple_of(part * half + c * kc, kc), kc)
            xs = recv[part, :, :, cols].reshape(slots, kc)
            acc_g[...] += dot_nt(xs, vg[:, wide])
            acc_u[...] += dot_nt(xs, vu[:, wide])

    project_part(tp)

    for q in range(1, group):
        part = lax.rem(tp + q, group)

        @pl.loop(0, experts)
        def _(k):
            forward(part, lax.rem(me + experts - k, experts), q).wait_recv()

        project_part(part)

    hbuf[tp] = silu_mul(acc_g[...], acc_u[...]).astype(BF16)
    swap_start(hbuf, 1)
    loads[4].wait()
    swap_recv(hbuf, 1)

    def down(hidden, weights, cols):
        depth = weights.shape[0] // group
        return sum(
            dot_nn(hidden[p], weights[p * depth : (p + 1) * depth, cols]) for p in range(group)
        )

    for c in range(half // kc):
        cols = slice(c * kc, (c + 1) * kc)
        outb[:, :, cols] = (
            down(hbuf, vd, cols).astype(BF16).reshape(experts, pad, kc)
        )

    @pl.loop(1, experts)
    def _(k):
        give_back(lax.rem(me + k, experts), me).start()

    own_back = pltpu.make_async_copy(
        outb.at[me], ret.at[me], lsem.at[1]
    )
    own_back.start()

    loads[5].wait()
    swap_recv(shbuf, 0)
    for c in range(half // kc):
        cols = slice(c * kc, (c + 1) * kc)
        comb[:, cols] = down(shbuf, vsd, cols)
    spread = (
        lax.broadcasted_iota(jnp.int32, (experts, slots), 1) // pad
        == lax.broadcasted_iota(jnp.int32, (experts, slots), 0)
    ).astype(F32).astype(BF16)
    place = (lax.broadcasted_iota(jnp.int32, (rows, slots), 1) % pad).astype(F32)
    taken = (dot_nn(chosen, spread) > 0.5) & (dot_nn(rank, spread) == place)
    coarse = weight.astype(BF16)
    fine = (weight - coarse.astype(F32)).astype(BF16)
    mix_coarse = jnp.where(taken, dot_nn(coarse, spread), 0.0).astype(BF16)
    mix_fine = jnp.where(taken, dot_nn(fine, spread), 0.0).astype(BF16)

    own_back.wait()

    @pl.loop(1, experts)
    def _(k):
        source = lax.rem(me + experts - k, experts)
        give_back(source, source).wait_recv()

    total = jnp.zeros((rows, 1), F32)
    for c in range(half // kc):
        cols = slice(c * kc, (c + 1) * kc)
        back = ret[:, :, cols].reshape(slots, kc)
        part = comb[:, cols] + dot_nn(mix_coarse, back) + dot_nn(mix_fine, back)
        comb[:, cols] = part
        total = total + jnp.sum(part * part, axis=1, keepdims=True)
    sq[tp] = jnp.broadcast_to(total, sq.shape[1:])
    swap_start(sq, 2)

    @pl.loop(1, experts)
    def _(k):
        dest = lax.rem(me + k, experts)
        dispatch(dest, me).wait_send()
        give_back(dest, me).wait_send()

    @pl.loop(0, experts)
    def _(k):
        for q in range(1, group):
            forward(tp, k, q).wait_send()

    swap_sent(shbuf, 0)
    swap_sent(hbuf, 1)
    swap_recv(sq, 2)
    norm = lax.rsqrt(sum(sq[p] for p in range(group))[:, :1] / width + EPS)
    o[...] = (comb[...] * norm * outg[...]).astype(BF16)
    swap_sent(sq, 2)


def on_device(experts, tokens, in_gain, routes, gates, eg, eu, ed, sg, su, sd, out_gain):
    rows, width = tokens.shape
    group = lax.axis_size("tp")
    half = width // group
    cap = min(rows, (rows * routes.shape[1] + experts - 1) // experts + 1)
    pad = -(-cap // 16) * 16
    slots = experts * pad
    hid, shid = eg.shape[1], sg.shape[0]
    vmem = pl.BlockSpec(memory_space=pltpu.VMEM)
    hbm = pl.BlockSpec(memory_space=pl.ANY)
    dma = pltpu.SemaphoreType.DMA
    return pl.pallas_call(
        functools.partial(kernel, experts, cap, pad),
        out_shape=jax.ShapeDtypeStruct((rows, half), BF16),
        in_specs=[vmem] * 4 + [hbm] * 6 + [vmem],
        out_specs=vmem,
        scratch_shapes=[
            pltpu.VMEM(eg.shape[1:], BF16),
            pltpu.VMEM(eu.shape[1:], BF16),
            pltpu.VMEM(ed.shape[1:], BF16),
            pltpu.VMEM(sg.shape, BF16),
            pltpu.VMEM(su.shape, BF16),
            pltpu.VMEM(sd.shape, BF16),
            pltpu.VMEM((group, rows, half), BF16),
            pltpu.VMEM((experts, pad, half), BF16),
            pltpu.VMEM((group, experts, pad, half), BF16),
            pltpu.VMEM((slots, hid), F32),
            pltpu.VMEM((slots, hid), F32),
            pltpu.VMEM((rows, shid), F32),
            pltpu.VMEM((rows, shid), F32),
            pltpu.VMEM((group, slots, hid), BF16),
            pltpu.VMEM((group, rows, shid), BF16),
            pltpu.VMEM((experts, pad, half), BF16),
            pltpu.VMEM((experts, pad, half), BF16),
            pltpu.VMEM((rows, half), F32),
            pltpu.VMEM((group, rows, 128), F32),
            dma((6,)),
            dma((2,)),
            dma((experts,)),
            dma((experts,)),
            dma((group, experts)),
            dma((group, experts)),
            dma((experts,)),
            dma((experts,)),
            dma((3, group)),
            dma((3, group)),
        ],
        compiler_params=pltpu.CompilerParams(
            collective_id=0, has_side_effects=True, vmem_limit_bytes=60 * 1024 * 1024
        ),
    )(
        tokens, in_gain.reshape(1, width), routes, gates, eg, eu, ed, sg, su, sd,
        out_gain.reshape(1, half),
    )


def solution(mesh):
    in_specs = (
        P("ep", None),
        P(),
        P("ep", None),
        P("ep", None),
        P("ep", "tp", None),
        P("ep", "tp", None),
        P("ep", None, "tp"),
        P("tp", None),
        P("tp", None),
        P(None, "tp"),
        P("tp"),
    )
    return jax.shard_map(
        functools.partial(on_device, mesh.shape["ep"]),
        mesh=mesh,
        in_specs=in_specs,
        out_specs=P("ep", "tp"),
        check_vma=False,
    )
```

```python
import functools

import jax
import jax.numpy as jnp
from jax import lax
from jax.experimental import pallas as pl
from jax.experimental.pallas import tpu as pltpu
from jax.sharding import PartitionSpec as P

EPS = 1e-06
MESH = pl.DeviceIdType.MESH
F32 = jnp.float32
BF16 = jnp.bfloat16


def dot_nt(a, b):
    return lax.dot_general(a, b, (((1,), (1,)), ((), ())), preferred_element_type=F32)


def dot_nn(a, b):
    return jnp.dot(a, b, preferred_element_type=F32)


def silu_mul(g, u):
    return g / (1.0 + jnp.exp(-g)) * u


def kernel(
    experts, fulls, rest,
    tok, ing, routes, gates, eg, eu, ed, sg, su, sd, outg,
    o,
    vg, vu, vd, vsg, vsu, vsd,
    nrm, send, recv, acc_g, acc_u, sacc_g, sacc_u, hbuf, shbuf, outb, ret, comb, sq,
    wsem, lsem, dsend, drecv, fsend, frecv, rsend, rrecv, xsend, xrecv,
):
    me = lax.axis_index("ep")
    tp = lax.axis_index("tp")
    rows, width = tok.shape
    group = lax.axis_size("tp")
    half = width // group
    slots = experts * 8
    folds = 8 // rest if rest else 1
    kc = half // folds if rest else min(512, half)
    blocks = fulls + (1 if rest else 0)

    loads = [
        pltpu.make_async_copy(src, dst, wsem.at[i])
        for i, (src, dst) in enumerate(
            ((sg, vsg), (su, vsu), (eg.at[0], vg), (eu.at[0], vu), (ed.at[0], vd), (sd, vsd))
        )
    ]
    for load in loads:
        load.start()

    barrier = pltpu.get_barrier_semaphore()

    @pl.loop(1, experts)
    def _(k):
        pl.semaphore_signal(
            barrier, inc=1, device_id=(lax.rem(me + k, experts), tp), device_id_type=MESH
        )

    for q in range(1, group):
        pl.semaphore_signal(
            barrier, inc=1, device_id=(me, lax.rem(tp + q, group)), device_id_type=MESH
        )

    x = tok[...].astype(F32)
    scale = lax.rsqrt(jnp.mean(x * x, axis=1, keepdims=True) + EPS)
    for h in range(group):
        cols = slice(h * half, (h + 1) * half)
        nrm[h] = (tok[:, cols].astype(F32) * scale * ing[:, cols]).astype(BF16)

    expert_ids = lax.broadcasted_iota(jnp.int32, (experts, rows), 0)
    chosen_t = jnp.zeros((experts, rows), F32)
    weight_t = jnp.zeros((experts, rows), F32)
    for k in range(routes.shape[0]):
        hit = routes[k : k + 1, :] == expert_ids
        chosen_t = jnp.where(hit, 1.0, chosen_t)
        weight_t = jnp.where(hit, gates[k : k + 1, :], weight_t)
    chosen_t = chosen_t.astype(BF16)
    token_r = lax.broadcasted_iota(jnp.int32, (rows, rows), 0)
    token_c = lax.broadcasted_iota(jnp.int32, (rows, rows), 1)
    earlier = (token_r < token_c).astype(F32).astype(BF16)
    rank_t = dot_nn(chosen_t, earlier).astype(BF16)

    def places(slot):
        row = slot % 8
        listed = [((8 * i + row).astype(F32), None) for i in range(fulls)]
        if rest:
            listed.append(((8 * fulls + row % rest).astype(F32), row // rest))
        return listed

    spread_t = (
        lax.broadcasted_iota(jnp.int32, (slots, experts), 0) // 8
        == lax.broadcasted_iota(jnp.int32, (slots, experts), 1)
    ).astype(F32).astype(BF16)
    named_t = dot_nn(spread_t, chosen_t) > 0.5
    ranks_t = dot_nn(spread_t, rank_t)
    for i, (place, piece) in enumerate(
        places(lax.broadcasted_iota(jnp.int32, (slots, rows), 0))
    ):
        here = jnp.where(named_t & (ranks_t == place), 1.0, 0.0)
        if piece is None:
            here = here.astype(BF16)
            for c in range(half // kc):
                send[:, i * half + c * kc : i * half + (c + 1) * kc] = dot_nn(
                    here, nrm[tp, :, c * kc : (c + 1) * kc]
                ).astype(BF16)
        else:
            send[:, i * half : i * half + kc] = sum(
                dot_nn(
                    jnp.where(piece == c, here, 0.0).astype(BF16),
                    nrm[tp, :, c * kc : (c + 1) * kc],
                )
                for c in range(folds)
            ).astype(BF16)

    def own_rows(expert):
        return pl.ds(pl.multiple_of(expert * 8, 8), 8)

    pl.semaphore_wait(barrier, experts - 1 + group - 1)

    def dispatch(dest, source):
        return pltpu.make_async_remote_copy(
            src_ref=send.at[own_rows(dest)],
            dst_ref=recv.at[tp, own_rows(source)],
            send_sem=dsend.at[dest],
            recv_sem=drecv.at[source],
            device_id=(dest, tp),
            device_id_type=MESH,
        )

    def forward(part, source, q):
        return pltpu.make_async_remote_copy(
            src_ref=recv.at[part, own_rows(source)],
            dst_ref=recv.at[part, own_rows(source)],
            send_sem=fsend.at[q, source],
            recv_sem=frecv.at[part, source],
            device_id=(me, lax.rem(tp + q, group)),
            device_id_type=MESH,
        )

    def give_back(dest, source):
        return pltpu.make_async_remote_copy(
            src_ref=outb.at[own_rows(dest)],
            dst_ref=ret.at[own_rows(source)],
            send_sem=rsend.at[dest],
            recv_sem=rrecv.at[source],
            device_id=(dest, tp),
            device_id_type=MESH,
        )

    def swap(ref, i, part, q):
        return pltpu.make_async_remote_copy(
            src_ref=ref.at[part],
            dst_ref=ref.at[part],
            send_sem=xsend.at[i, q],
            recv_sem=xrecv.at[i, part],
            device_id=(me, lax.rem(tp + q, group)),
            device_id_type=MESH,
        )

    def swap_start(ref, i):
        for q in range(1, group):
            swap(ref, i, tp, q).start()

    def swap_recv(ref, i):
        for q in range(1, group):
            swap(ref, i, lax.rem(tp + q, group), q).wait_recv()

    def swap_sent(ref, i):
        for q in range(1, group):
            swap(ref, i, tp, q).wait_send()

    def forward_start(source):
        for q in range(1, group):
            forward(tp, source, q).start()

    @pl.loop(1, experts)
    def _(k):
        dispatch(lax.rem(me + k, experts), me).start()

    own = pltpu.make_async_copy(
        send.at[own_rows(me)], recv.at[tp, own_rows(me)], lsem.at[0]
    )
    own.start()

    loads[0].wait()
    loads[1].wait()
    sacc_g[...] = jnp.zeros_like(sacc_g)
    sacc_u[...] = jnp.zeros_like(sacc_u)
    for h in range(group):

        @pl.loop(0, half // kc)
        def _(c):
            cols = pl.ds(pl.multiple_of(c * kc, kc), kc)
            wide = pl.ds(pl.multiple_of(h * half + c * kc, kc), kc)
            xs = nrm[h, :, cols]
            sacc_g[...] += dot_nt(xs, vsg[:, wide])
            sacc_u[...] += dot_nt(xs, vsu[:, wide])

    shbuf[tp] = silu_mul(sacc_g[...], sacc_u[...]).astype(BF16)
    swap_start(shbuf, 0)

    own.wait()
    forward_start(me)

    @pl.loop(1, experts)
    def _(k):
        source = lax.rem(me + experts - k, experts)
        dispatch(source, source).wait_recv()
        forward_start(source)

    loads[2].wait()
    loads[3].wait()
    acc_g[...] = jnp.zeros_like(acc_g)
    acc_u[...] = jnp.zeros_like(acc_u)

    if rest:
        row_piece = lax.broadcasted_iota(jnp.int32, (slots, kc), 0) % 8 // rest

    def project_part(part):
        @pl.loop(0, half // kc)
        def _(c):
            cols = pl.ds(pl.multiple_of(c * kc, kc), kc)
            wide = pl.ds(pl.multiple_of(part * half + c * kc, kc), kc)
            pieces = [
                recv[part, :, pl.ds(pl.multiple_of(i * half + c * kc, kc), kc)]
                for i in range(fulls)
            ]
            if rest:
                last = recv[part, :, fulls * half : fulls * half + kc]
                pieces.append(jnp.where(row_piece == c, last, jnp.zeros_like(last)))
            xs = jnp.concatenate(pieces, axis=0)
            acc_g[...] += dot_nt(xs, vg[:, wide])
            acc_u[...] += dot_nt(xs, vu[:, wide])

    project_part(tp)

    for q in range(1, group):
        part = lax.rem(tp + q, group)

        @pl.loop(0, experts)
        def _(k):
            forward(part, lax.rem(me + experts - k, experts), q).wait_recv()

        project_part(part)

    for i in range(blocks):
        block = slice(i * slots, (i + 1) * slots)
        g, u = acc_g[block], acc_u[block]
        if i == fulls:
            g = g.reshape(experts, 8, -1)
            u = u.reshape(experts, 8, -1)
            shift = rest
            while shift < 8:
                g = g + pltpu.roll(g, shift, 1)
                u = u + pltpu.roll(u, shift, 1)
                shift *= 2
            g = g.reshape(slots, -1)
            u = u.reshape(slots, -1)
        hbuf[tp, block] = silu_mul(g, u).astype(BF16)
    swap_start(hbuf, 1)
    loads[4].wait()
    swap_recv(hbuf, 1)

    def down(hidden, weights, cols):
        depth = weights.shape[0] // group
        return sum(
            dot_nn(hidden[p], weights[p * depth : (p + 1) * depth, cols]) for p in range(group)
        )

    for c in range(half // kc):
        cols = slice(c * kc, (c + 1) * kc)
        made = down(hbuf, vd, cols)
        for i in range(fulls):
            outb[:, i * half + c * kc : i * half + (c + 1) * kc] = made[
                i * slots : (i + 1) * slots
            ].astype(BF16)
        if rest:
            fresh = made[fulls * slots :]
            last = fresh if c == 0 else jnp.where(row_piece == c, fresh, last)
    if rest:
        outb[:, fulls * half :] = last.astype(BF16)

    @pl.loop(1, experts)
    def _(k):
        give_back(lax.rem(me + k, experts), me).start()

    own_back = pltpu.make_async_copy(
        outb.at[own_rows(me)], ret.at[own_rows(me)], lsem.at[1]
    )
    own_back.start()

    loads[5].wait()
    swap_recv(shbuf, 0)
    for c in range(half // kc):
        cols = slice(c * kc, (c + 1) * kc)
        comb[:, cols] = down(shbuf, vsd, cols)
    spread = (
        lax.broadcasted_iota(jnp.int32, (experts, slots), 1) // 8
        == lax.broadcasted_iota(jnp.int32, (experts, slots), 0)
    ).astype(F32).astype(BF16)
    eye = (token_r == token_c).astype(F32).astype(BF16)
    coarse_t = weight_t.astype(BF16)
    fine_t = (weight_t - coarse_t.astype(F32)).astype(BF16)
    named, ranks, coarse, fine = [
        dot_nn(dot_nt(eye, t).astype(BF16), spread) for t in (chosen_t, rank_t, coarse_t, fine_t)
    ]
    mixing = []
    for place, piece in places(lax.broadcasted_iota(jnp.int32, (rows, slots), 1)):
        taken = (named > 0.5) & (ranks == place)
        mixing.append((taken, piece))

    own_back.wait()

    @pl.loop(1, experts)
    def _(k):
        source = lax.rem(me + experts - k, experts)
        give_back(source, source).wait_recv()

    total = jnp.zeros((rows, 1), F32)
    for c in range(half // kc):
        cols = slice(c * kc, (c + 1) * kc)
        part = comb[:, cols]
        for i, (taken, piece) in enumerate(mixing):
            if piece is None:
                back = ret[:, i * half + c * kc : i * half + (c + 1) * kc]
            else:
                back = ret[:, i * half : i * half + kc]
                taken = taken & (piece == c)
            part += dot_nn(jnp.where(taken, coarse, 0.0).astype(BF16), back)
            part += dot_nn(jnp.where(taken, fine, 0.0).astype(BF16), back)
        comb[:, cols] = part
        total = total + jnp.sum(part * part, axis=1, keepdims=True)
    sq[tp] = jnp.broadcast_to(total, sq.shape[1:])
    swap_start(sq, 2)

    @pl.loop(1, experts)
    def _(k):
        dest = lax.rem(me + k, experts)
        dispatch(dest, me).wait_send()
        give_back(dest, me).wait_send()

    @pl.loop(0, experts)
    def _(k):
        for q in range(1, group):
            forward(tp, k, q).wait_send()

    swap_sent(shbuf, 0)
    swap_sent(hbuf, 1)
    swap_recv(sq, 2)
    norm = lax.rsqrt(sum(sq[p] for p in range(group))[:, :1] / width + EPS)
    o[...] = (comb[...] * norm * outg[...]).astype(BF16)
    swap_sent(sq, 2)


def on_device(experts, tokens, in_gain, routes, gates, eg, eu, ed, sg, su, sd, out_gain):
    rows, width = tokens.shape
    group = lax.axis_size("tp")
    half = width // group
    cap = min(rows, (rows * routes.shape[1] + experts - 1) // experts + 1)
    fulls, rest = cap // 8, cap % 8
    while rest & (rest - 1):
        rest += 1
    if rest and half * rest // 8 % 128:
        rest = 8
    if rest == 8:
        fulls, rest = fulls + 1, 0
    slots = experts * 8
    blocks = fulls + (1 if rest else 0)
    packed = fulls * half + half * rest // 8
    hid, shid = eg.shape[1], sg.shape[0]
    vmem = pl.BlockSpec(memory_space=pltpu.VMEM)
    hbm = pl.BlockSpec(memory_space=pl.ANY)
    dma = pltpu.SemaphoreType.DMA
    return pl.pallas_call(
        functools.partial(kernel, experts, fulls, rest),
        out_shape=jax.ShapeDtypeStruct((rows, half), BF16),
        in_specs=[vmem] * 4 + [hbm] * 6 + [vmem],
        out_specs=vmem,
        scratch_shapes=[
            pltpu.VMEM(eg.shape[1:], BF16),
            pltpu.VMEM(eu.shape[1:], BF16),
            pltpu.VMEM(ed.shape[1:], BF16),
            pltpu.VMEM(sg.shape, BF16),
            pltpu.VMEM(su.shape, BF16),
            pltpu.VMEM(sd.shape, BF16),
            pltpu.VMEM((group, rows, half), BF16),
            pltpu.VMEM((slots, packed), BF16),
            pltpu.VMEM((group, slots, packed), BF16),
            pltpu.VMEM((blocks * slots, hid), F32),
            pltpu.VMEM((blocks * slots, hid), F32),
            pltpu.VMEM((rows, shid), F32),
            pltpu.VMEM((rows, shid), F32),
            pltpu.VMEM((group, blocks * slots, hid), BF16),
            pltpu.VMEM((group, rows, shid), BF16),
            pltpu.VMEM((slots, packed), BF16),
            pltpu.VMEM((slots, packed), BF16),
            pltpu.VMEM((rows, half), F32),
            pltpu.VMEM((group, rows, 128), F32),
            dma((6,)),
            dma((2,)),
            dma((experts,)),
            dma((experts,)),
            dma((group, experts)),
            dma((group, experts)),
            dma((experts,)),
            dma((experts,)),
            dma((3, group)),
            dma((3, group)),
        ],
        compiler_params=pltpu.CompilerParams(
            collective_id=0, has_side_effects=True, vmem_limit_bytes=60 * 1024 * 1024
        ),
    )(
        tokens, in_gain.reshape(1, width), routes.T, gates.T, eg, eu, ed, sg, su, sd,
        out_gain.reshape(1, half),
    )


def solution(mesh):
    in_specs = (
        P("ep", None),
        P(),
        P("ep", None),
        P("ep", None),
        P("ep", "tp", None),
        P("ep", "tp", None),
        P("ep", None, "tp"),
        P("tp", None),
        P("tp", None),
        P(None, "tp"),
        P("tp"),
    )
    return jax.shard_map(
        functools.partial(on_device, mesh.shape["ep"]),
        mesh=mesh,
        in_specs=in_specs,
        out_specs=P("ep", "tp"),
        check_vma=False,
    )
```

```python
import functools

import jax
import jax.numpy as jnp
from jax import lax
from jax.experimental import pallas as pl
from jax.experimental.pallas import tpu as pltpu
from jax.sharding import PartitionSpec as P

EPS = 1e-06
MESH = pl.DeviceIdType.MESH
F32 = jnp.float32
BF16 = jnp.bfloat16


def dot_nt(a, b):
    return lax.dot_general(a, b, (((1,), (1,)), ((), ())), preferred_element_type=F32)


def dot_nn(a, b):
    return jnp.dot(a, b, preferred_element_type=F32)


def silu_mul(g, u):
    return g / (1.0 + jnp.exp(-g)) * u


def kernel(
    experts, fulls, rest,
    tok, ing, routes, gates, eg, eu, ed, sg, su, sd, outg,
    o,
    vg, vu, vd, vsg, vsu, vsd,
    nrm, send, recv, acc_g, acc_u, sacc_g, sacc_u, hbuf, shbuf, outb, ret, comb, sq,
    wsem, lsem, dsend, drecv, fsend, frecv, rsend, rrecv, xsend, xrecv,
):
    me = lax.axis_index("ep")
    tp = lax.axis_index("tp")
    rows, width = tok.shape
    group = lax.axis_size("tp")
    half = width // group
    slots = experts * 8
    folds = 8 // rest if rest else 1
    kc = half // folds if rest else min(512, half)
    blocks = fulls + (1 if rest else 0)

    loads = [
        pltpu.make_async_copy(src, dst, wsem.at[i])
        for i, (src, dst) in enumerate(
            ((sg, vsg), (su, vsu), (eg.at[0], vg), (eu.at[0], vu), (ed.at[0], vd), (sd, vsd))
        )
    ]
    for load in loads:
        load.start()

    barrier = pltpu.get_barrier_semaphore()

    @pl.loop(1, experts)
    def _(k):
        pl.semaphore_signal(
            barrier, inc=1, device_id=(lax.rem(me + k, experts), tp), device_id_type=MESH
        )

    for q in range(1, group):
        pl.semaphore_signal(
            barrier, inc=1, device_id=(me, lax.rem(tp + q, group)), device_id_type=MESH
        )

    x = tok[...].astype(F32)
    scale = lax.rsqrt(jnp.mean(x * x, axis=1, keepdims=True) + EPS)

    def normalize(part):
        cols = pl.ds(pl.multiple_of(part * half, half), half)
        nrm[part] = (tok[:, cols].astype(F32) * scale * ing[:, cols]).astype(BF16)

    normalize(tp)

    expert_ids = lax.broadcasted_iota(jnp.int32, (experts, rows), 0)
    chosen_t = jnp.zeros((experts, rows), F32)
    weight_t = jnp.zeros((experts, rows), F32)
    for k in range(routes.shape[0]):
        hit = routes[k : k + 1, :] == expert_ids
        chosen_t = jnp.where(hit, 1.0, chosen_t)
        weight_t = jnp.where(hit, gates[k : k + 1, :], weight_t)
    chosen_t = chosen_t.astype(BF16)
    token_r = lax.broadcasted_iota(jnp.int32, (rows, rows), 0)
    token_c = lax.broadcasted_iota(jnp.int32, (rows, rows), 1)
    earlier = (token_r < token_c).astype(F32).astype(BF16)
    rank_t = dot_nn(chosen_t, earlier).astype(BF16)

    def places(slot):
        row = slot % 8
        listed = [((8 * i + row).astype(F32), None) for i in range(fulls)]
        if rest:
            listed.append(((8 * fulls + row % rest).astype(F32), row // rest))
        return listed

    spread_t = (
        lax.broadcasted_iota(jnp.int32, (slots, experts), 0) // 8
        == lax.broadcasted_iota(jnp.int32, (slots, experts), 1)
    ).astype(F32).astype(BF16)
    named_t = dot_nn(spread_t, chosen_t) > 0.5
    ranks_t = dot_nn(spread_t, rank_t)
    for i, (place, piece) in enumerate(
        places(lax.broadcasted_iota(jnp.int32, (slots, rows), 0))
    ):
        here = jnp.where(named_t & (ranks_t == place), 1.0, 0.0)
        if piece is None:
            here = here.astype(BF16)
            for c in range(half // kc):
                send[:, i * half + c * kc : i * half + (c + 1) * kc] = dot_nn(
                    here, nrm[tp, :, c * kc : (c + 1) * kc]
                ).astype(BF16)
        else:
            send[:, i * half : i * half + kc] = sum(
                dot_nn(
                    jnp.where(piece == c, here, 0.0).astype(BF16),
                    nrm[tp, :, c * kc : (c + 1) * kc],
                )
                for c in range(folds)
            ).astype(BF16)

    def own_rows(expert):
        return pl.ds(pl.multiple_of(expert * 8, 8), 8)

    pl.semaphore_wait(barrier, experts - 1 + group - 1)

    def dispatch(dest, source):
        return pltpu.make_async_remote_copy(
            src_ref=send.at[own_rows(dest)],
            dst_ref=recv.at[tp, own_rows(source)],
            send_sem=dsend.at[dest],
            recv_sem=drecv.at[source],
            device_id=(dest, tp),
            device_id_type=MESH,
        )

    def forward(part, source, q):
        return pltpu.make_async_remote_copy(
            src_ref=recv.at[part, own_rows(source)],
            dst_ref=recv.at[part, own_rows(source)],
            send_sem=fsend.at[q, source],
            recv_sem=frecv.at[part, source],
            device_id=(me, lax.rem(tp + q, group)),
            device_id_type=MESH,
        )

    def give_back(dest, source):
        return pltpu.make_async_remote_copy(
            src_ref=outb.at[own_rows(dest)],
            dst_ref=ret.at[own_rows(source)],
            send_sem=rsend.at[dest],
            recv_sem=rrecv.at[source],
            device_id=(dest, tp),
            device_id_type=MESH,
        )

    def swap(ref, i, part, q):
        return pltpu.make_async_remote_copy(
            src_ref=ref.at[part],
            dst_ref=ref.at[part],
            send_sem=xsend.at[i, q],
            recv_sem=xrecv.at[i, part],
            device_id=(me, lax.rem(tp + q, group)),
            device_id_type=MESH,
        )

    def swap_start(ref, i):
        for q in range(1, group):
            swap(ref, i, tp, q).start()

    def swap_recv(ref, i):
        for q in range(1, group):
            swap(ref, i, lax.rem(tp + q, group), q).wait_recv()

    def swap_sent(ref, i):
        for q in range(1, group):
            swap(ref, i, tp, q).wait_send()

    def forward_start(source):
        for q in range(1, group):
            forward(tp, source, q).start()

    @pl.loop(1, experts)
    def _(k):
        dispatch(lax.rem(me + k, experts), me).start()

    own = pltpu.make_async_copy(
        send.at[own_rows(me)], recv.at[tp, own_rows(me)], lsem.at[0]
    )
    own.start()

    for q in range(1, group):
        normalize(lax.rem(tp + q, group))
    loads[0].wait()
    loads[1].wait()
    sacc_g[...] = jnp.zeros_like(sacc_g)
    sacc_u[...] = jnp.zeros_like(sacc_u)
    for h in range(group):

        @pl.loop(0, half // kc)
        def _(c):
            cols = pl.ds(pl.multiple_of(c * kc, kc), kc)
            wide = pl.ds(pl.multiple_of(h * half + c * kc, kc), kc)
            xs = nrm[h, :, cols]
            sacc_g[...] += dot_nt(xs, vsg[:, wide])
            sacc_u[...] += dot_nt(xs, vsu[:, wide])

    shbuf[tp] = silu_mul(sacc_g[...], sacc_u[...]).astype(BF16)
    swap_start(shbuf, 0)

    own.wait()
    forward_start(me)

    @pl.loop(1, experts)
    def _(k):
        source = lax.rem(me + experts - k, experts)
        dispatch(source, source).wait_recv()
        forward_start(source)

    loads[2].wait()
    loads[3].wait()
    acc_g[...] = jnp.zeros_like(acc_g)
    acc_u[...] = jnp.zeros_like(acc_u)

    if rest:
        row_piece = lax.broadcasted_iota(jnp.int32, (slots, kc), 0) % 8 // rest

    def project_part(part):
        @pl.loop(0, half // kc)
        def _(c):
            cols = pl.ds(pl.multiple_of(c * kc, kc), kc)
            wide = pl.ds(pl.multiple_of(part * half + c * kc, kc), kc)
            pieces = [
                recv[part, :, pl.ds(pl.multiple_of(i * half + c * kc, kc), kc)]
                for i in range(fulls)
            ]
            if rest:
                last = recv[part, :, fulls * half : fulls * half + kc]
                pieces.append(jnp.where(row_piece == c, last, jnp.zeros_like(last)))
            xs = jnp.concatenate(pieces, axis=0)
            acc_g[...] += dot_nt(xs, vg[:, wide])
            acc_u[...] += dot_nt(xs, vu[:, wide])

    project_part(tp)

    for q in range(1, group):
        part = lax.rem(tp + q, group)

        @pl.loop(0, experts)
        def _(k):
            forward(part, lax.rem(me + experts - k, experts), q).wait_recv()

        project_part(part)

    for i in range(blocks):
        block = slice(i * slots, (i + 1) * slots)
        g, u = acc_g[block], acc_u[block]
        if i == fulls:
            g = g.reshape(experts, 8, -1)
            u = u.reshape(experts, 8, -1)
            shift = rest
            while shift < 8:
                g = g + pltpu.roll(g, shift, 1)
                u = u + pltpu.roll(u, shift, 1)
                shift *= 2
            g = g.reshape(slots, -1)
            u = u.reshape(slots, -1)
        hbuf[tp, block] = silu_mul(g, u).astype(BF16)
    swap_start(hbuf, 1)
    loads[4].wait()
    swap_recv(hbuf, 1)

    def down(hidden, weights, cols):
        depth = weights.shape[0] // group
        return sum(
            dot_nn(hidden[p], weights[p * depth : (p + 1) * depth, cols]) for p in range(group)
        )

    for c in range(half // kc):
        cols = slice(c * kc, (c + 1) * kc)
        made = down(hbuf, vd, cols)
        for i in range(fulls):
            outb[:, i * half + c * kc : i * half + (c + 1) * kc] = made[
                i * slots : (i + 1) * slots
            ].astype(BF16)
        if rest:
            fresh = made[fulls * slots :]
            last = fresh if c == 0 else jnp.where(row_piece == c, fresh, last)
    if rest:
        outb[:, fulls * half :] = last.astype(BF16)

    @pl.loop(1, experts)
    def _(k):
        give_back(lax.rem(me + k, experts), me).start()

    own_back = pltpu.make_async_copy(
        outb.at[own_rows(me)], ret.at[own_rows(me)], lsem.at[1]
    )
    own_back.start()

    loads[5].wait()
    swap_recv(shbuf, 0)
    for c in range(half // kc):
        cols = slice(c * kc, (c + 1) * kc)
        comb[:, cols] = down(shbuf, vsd, cols)
    spread = (
        lax.broadcasted_iota(jnp.int32, (experts, slots), 1) // 8
        == lax.broadcasted_iota(jnp.int32, (experts, slots), 0)
    ).astype(F32).astype(BF16)
    eye = (token_r == token_c).astype(F32).astype(BF16)
    coarse_t = weight_t.astype(BF16)
    fine_t = (weight_t - coarse_t.astype(F32)).astype(BF16)
    named, ranks, coarse, fine = [
        dot_nn(dot_nt(eye, t).astype(BF16), spread) for t in (chosen_t, rank_t, coarse_t, fine_t)
    ]
    mixing = []
    for place, piece in places(lax.broadcasted_iota(jnp.int32, (rows, slots), 1)):
        taken = (named > 0.5) & (ranks == place)
        mixing.append((taken, piece))

    own_back.wait()

    @pl.loop(1, experts)
    def _(k):
        source = lax.rem(me + experts - k, experts)
        give_back(source, source).wait_recv()

    total = jnp.zeros((rows, 1), F32)
    for c in range(half // kc):
        cols = slice(c * kc, (c + 1) * kc)
        part = comb[:, cols]
        for i, (taken, piece) in enumerate(mixing):
            if piece is None:
                back = ret[:, i * half + c * kc : i * half + (c + 1) * kc]
            else:
                back = ret[:, i * half : i * half + kc]
                taken = taken & (piece == c)
            both = jnp.concatenate(
                [jnp.where(taken, coarse, 0.0), jnp.where(taken, fine, 0.0)], axis=0
            )
            mixed = dot_nn(both.astype(BF16), back)
            part += mixed[:rows] + mixed[rows:]
        comb[:, cols] = part
        total = total + jnp.sum(part * part, axis=1, keepdims=True)
    sq[tp] = jnp.broadcast_to(total, sq.shape[1:])
    swap_start(sq, 2)

    @pl.loop(1, experts)
    def _(k):
        dest = lax.rem(me + k, experts)
        dispatch(dest, me).wait_send()
        give_back(dest, me).wait_send()

    @pl.loop(0, experts)
    def _(k):
        for q in range(1, group):
            forward(tp, k, q).wait_send()

    swap_sent(shbuf, 0)
    swap_sent(hbuf, 1)
    swap_recv(sq, 2)
    norm = lax.rsqrt(sum(sq[p] for p in range(group))[:, :1] / width + EPS)
    o[...] = (comb[...] * norm * outg[...]).astype(BF16)
    swap_sent(sq, 2)


def on_device(experts, tokens, in_gain, routes, gates, eg, eu, ed, sg, su, sd, out_gain):
    rows, width = tokens.shape
    group = lax.axis_size("tp")
    half = width // group
    cap = min(rows, (rows * routes.shape[1] + experts - 1) // experts + 1)
    fulls, rest = cap // 8, cap % 8
    while rest & (rest - 1):
        rest += 1
    if rest and half * rest // 8 % 128:
        rest = 8
    if rest == 8:
        fulls, rest = fulls + 1, 0
    slots = experts * 8
    blocks = fulls + (1 if rest else 0)
    packed = fulls * half + half * rest // 8
    hid, shid = eg.shape[1], sg.shape[0]
    vmem = pl.BlockSpec(memory_space=pltpu.VMEM)
    hbm = pl.BlockSpec(memory_space=pl.ANY)
    dma = pltpu.SemaphoreType.DMA
    return pl.pallas_call(
        functools.partial(kernel, experts, fulls, rest),
        out_shape=jax.ShapeDtypeStruct((rows, half), BF16),
        in_specs=[vmem] * 4 + [hbm] * 6 + [vmem],
        out_specs=vmem,
        scratch_shapes=[
            pltpu.VMEM(eg.shape[1:], BF16),
            pltpu.VMEM(eu.shape[1:], BF16),
            pltpu.VMEM(ed.shape[1:], BF16),
            pltpu.VMEM(sg.shape, BF16),
            pltpu.VMEM(su.shape, BF16),
            pltpu.VMEM(sd.shape, BF16),
            pltpu.VMEM((group, rows, half), BF16),
            pltpu.VMEM((slots, packed), BF16),
            pltpu.VMEM((group, slots, packed), BF16),
            pltpu.VMEM((blocks * slots, hid), F32),
            pltpu.VMEM((blocks * slots, hid), F32),
            pltpu.VMEM((rows, shid), F32),
            pltpu.VMEM((rows, shid), F32),
            pltpu.VMEM((group, blocks * slots, hid), BF16),
            pltpu.VMEM((group, rows, shid), BF16),
            pltpu.VMEM((slots, packed), BF16),
            pltpu.VMEM((slots, packed), BF16),
            pltpu.VMEM((rows, half), F32),
            pltpu.VMEM((group, rows, 128), F32),
            dma((6,)),
            dma((2,)),
            dma((experts,)),
            dma((experts,)),
            dma((group, experts)),
            dma((group, experts)),
            dma((experts,)),
            dma((experts,)),
            dma((3, group)),
            dma((3, group)),
        ],
        compiler_params=pltpu.CompilerParams(
            collective_id=0, has_side_effects=True, vmem_limit_bytes=60 * 1024 * 1024
        ),
    )(
        tokens, in_gain.reshape(1, width), routes.T, gates.T, eg, eu, ed, sg, su, sd,
        out_gain.reshape(1, half),
    )


def solution(mesh):
    in_specs = (
        P("ep", None),
        P(),
        P("ep", None),
        P("ep", None),
        P("ep", "tp", None),
        P("ep", "tp", None),
        P("ep", None, "tp"),
        P("tp", None),
        P("tp", None),
        P(None, "tp"),
        P("tp"),
    )
    return jax.shard_map(
        functools.partial(on_device, mesh.shape["ep"]),
        mesh=mesh,
        in_specs=in_specs,
        out_specs=P("ep", "tp"),
        check_vma=False,
    )
```
